512 devices in a mesh: ep: 16 (over y, x), tp: 32 (over z, core).
Axes of the slice: x: 4, y: 4, z: 16, core: 2. Of those that a mesh axis runs over, the one named last changes fastest.
Arguments:
- tokens: bfloat16 [8192, 4096], P('tp', 'ep'), may hold values from -20 to 20
- norm_gain: bfloat16 [4096], P('ep'), may hold values from 0.099609375 to 1.8984375
- expert_ids: int32 [8192, 2], P('tp'), may hold values from 0 to 31, all different within a row; in each aligned block of 256 rows (0 to 255, 256 to 511, ...) at most 32 rows name the same one
- combine_weight: float32 [8192, 2], P('tp'), may hold values from 0.05 to 1
- w_gate: bfloat16 [32, 2048, 4096], P('tp', 'ep'), may hold values from -0.09375 to 0.09375
- w_up: bfloat16 [32, 2048, 4096], P('tp', 'ep'), may hold values from -0.09375 to 0.09375
- w_down: bfloat16 [32, 2048, 4096], P('tp', None, 'ep'), may hold values from -2 to 2
- out_gain: bfloat16 [4096], P('ep'), may hold values from 0.099609375 to 1.8984375
Outputs:
- mixed: bfloat16 [8192, 4096], P('tp', 'ep')
The draws below stay inside these ranges and needn't reach their ends.
Inputs may be any that keep to these rules, and one draw needn't show every extreme that they name: `expert_ids`: each row names 2 different experts; among the rows of one index of tp no expert is named by more than 32 rows, a bound that some block reaches.
All inputs are finite; a program needn't handle non-finite values.
Results may differ from the reference program's by a relative error of at most 0.007.
Values may be sent and summed in bfloat16 or wider, within the bound.
No kernel may reach another device: no remote copies, remote signals or barrier semaphores. Data moves between devices by JAX's collectives and lax.ppermute only.
A program may use at most 64 MiB of HBM per device.

```python
import math
import jax
import jax.numpy as jnp
import numpy as np
from jax import lax

D = 4096
F = 2048
TOP = 2
TOK_DEV = 256
EXPERTS = 32
TOKENS = 8192
CAP = 32
N_TP = 32


def draw_tokens(key, part):
    first, second, third = jax.random.split(key, 3)
    block_scale = jnp.exp(jax.random.uniform(first, (D // 64,), jnp.float32, -1.1, 1.1))
    column_scale = jnp.repeat(block_scale, 64)
    base = jnp.clip(jax.random.normal(second, (TOKENS, D), jnp.float32), -6.0, 6.0)
    values = base * column_scale[None, :]
    return values.astype(jnp.bfloat16)


def draw_w_down(key, part):
    first, second = jax.random.split(key, 2)
    block_scale = jnp.exp(jax.random.uniform(first, (D // 64,), jnp.float32, -1.0, 1.0))
    column_scale = jnp.repeat(block_scale, 64)
    base = jnp.clip(jax.random.normal(second, (EXPERTS, F, D), jnp.float32), -4.0, 4.0)
    values = base * F ** (-0.5) * column_scale[None, None, :]
    return values.astype(jnp.bfloat16)


def levels(rng, shape, pieces, low, top_value):
    loudness, own = 1.0, jax.random.fold_in(rng, 6)
    for dim, blocks in pieces:
        heights = jnp.exp(jax.random.uniform(jax.random.fold_in(own, dim), (blocks,), jnp.float32, low / len(pieces), top_value / len(pieces)))
        loudness = loudness * jnp.repeat(heights, shape[dim] // blocks).reshape([-1 if axis == dim else 1 for axis in range(len(shape))])
    return loudness


def deal_out(own_key, own, number, rows, amount, top, bound, skew):
    ranking = jax.random.permutation(own_key, amount)
    heavy_load, usual = load_shares(amount, rows * top, bound, skew, True), load_shares(amount, rows * top, bound, skew, False)
    places = jnp.arange(amount)

    def named(lengths, turn):
        used = int((lengths > 0).sum())
        fixed = max(1, used // 4)
        passed = fixed + (places - fixed + turn * (used - fixed)) % max(1, amount - fixed)
        return jnp.zeros((amount,), jnp.int32).at[ranking[jnp.where(places < fixed, places, passed)]].set(jnp.asarray(lengths, jnp.int32))

    lengths = jnp.where(number % 4 == 0, named(heavy_load, number // 4), named(usual, number - number // 4 - 1))
    mixed = jax.random.permutation(jax.random.fold_in(own, 3), amount)
    giver, taker = mixed[0:amount // 2 * 2:2], mixed[1:amount // 2 * 2:2]
    slack = jnp.minimum(lengths[giver] - 1, bound - lengths[taker]) // 2
    slack = jnp.where((giver == ranking[0]) | (taker == ranking[0]) | (lengths[taker] == 0), 0, jnp.maximum(slack, 0))
    passed = jax.random.randint(jax.random.fold_in(own, 4), (amount // 2,), 0, 1 << 20) % (slack + 1)
    lengths = lengths.at[giver].add(-passed).at[taker].add(passed)
    items = jnp.searchsorted(jnp.cumsum(lengths), jnp.arange(rows * top), side="right").astype(jnp.int32)
    table = items.reshape(top, rows).T
    table = table[jax.random.permutation(jax.random.fold_in(own, 1), rows)]
    turn = jax.random.randint(jax.random.fold_in(own, 2), (rows, 1), 0, top)
    return jnp.take_along_axis(table, (jnp.arange(top)[None, :] + turn) % top, axis=1)


def load_shares(number_of, total, bound, skew, full):
    loads = [(1 << 20) // math.isqrt(rank ** skew) + 1 for rank in range(1, number_of + 1)]
    largest = bound if full else min(bound, max(-(-total // number_of), total * loads[0] // sum(loads)))
    least = 1 if total - largest >= number_of - 1 else 0
    given, rest = [largest] + [least] * (number_of - 1), total - largest - least * (number_of - 1)
    while rest > 0:
        movable = [i for i in range(1, number_of) if given[i] < largest] or [i for i in range(1, number_of) if given[i] < bound]
        whole, left = sum([loads[i] for i in movable]), rest
        for i in movable:
            addition = min(bound - given[i], max(1, left * loads[i] // whole), rest)
            given[i] = given[i] + addition
            rest = rest - addition
    return np.array(given)


def bell_draw(stream_key, shape, width, bound, shards=(), kind=jnp.bfloat16):
    result = width * jax.random.normal(stream_key, shape, jnp.float32)
    if shards:
        result = result * levels(stream_key, shape, shards, -0.22, 0.18)
    return jnp.clip(result, -bound, bound).astype(kind)


def setup_inputs(seed: int = 0) -> dict:
    key_of = jax.random.split(jax.random.key(seed), 9)
    tokens = draw_tokens(jax.random.fold_in(key_of[8], 71), 0)
    norm_gain = jnp.clip(1.0 + 0.18 * jax.random.normal(key_of[1], (D,), jnp.float32), 0.099609375, 1.8984375).astype(jnp.bfloat16)
    expert_ids_keys = jax.random.split(jax.random.fold_in(key_of[2], 1), TOKENS // TOK_DEV)
    expert_ids_turns = jax.random.permutation(jax.random.fold_in(key_of[2], 3), TOKENS // TOK_DEV)
    expert_ids = jax.vmap(lambda own, number: deal_out(jax.random.fold_in(key_of[2], 2), own, number, TOK_DEV, EXPERTS, TOP, CAP, 2))(expert_ids_keys, expert_ids_turns).reshape((TOKENS, TOP))
    combine_weight = jnp.clip(jnp.exp(math.log(1.0) - 2.9957323 * jax.random.uniform(key_of[3], (TOKENS, TOP), jnp.float32) ** levels(key_of[3], (TOKENS, TOP), ((0, 32),), -0.2, 0.2)), 0.05, 1.0)
    w_gate = bell_draw(key_of[4], (EXPERTS, F, D), D ** -0.5, 0.09375, ((0, 32), (1, 16)))
    w_up = bell_draw(key_of[5], (EXPERTS, F, D), D ** -0.5, 0.09375, ((0, 32), (1, 16)))
    w_down = draw_w_down(jax.random.fold_in(key_of[8], 71), 0)
    out_gain = jnp.clip(1.0 + 0.18 * jax.random.normal(key_of[7], (D,), jnp.float32), 0.099609375, 1.8984375).astype(jnp.bfloat16)
    return dict(tokens=tokens, norm_gain=norm_gain, expert_ids=expert_ids, combine_weight=combine_weight, w_gate=w_gate, w_up=w_up, w_down=w_down, out_gain=out_gain)


epsilon = 1e-06

def reference(tokens, norm_gain, expert_ids, combine_weight, w_gate, w_up, w_down, out_gain):
    xf = tokens.astype(jnp.float32)
    normed = (xf * lax.rsqrt(lax.optimization_barrier(jnp.mean(xf * xf, axis=1, keepdims=True)) + epsilon) * norm_gain.astype(jnp.float32)).astype(jnp.bfloat16)
    flat_ids = expert_ids.reshape(-1)
    flat_weight = combine_weight.reshape(-1)
    source_rows = (jnp.arange(TOKENS * TOP, dtype=jnp.int32) // TOP).astype(jnp.int32)
    most = N_TP * CAP

    def one_expert(carry, expert):
        mask = flat_ids == expert
        ranks = jnp.cumsum(mask.astype(jnp.int32)) - 1
        slots = jnp.where(mask, ranks, most).astype(jnp.int32)
        rows = jnp.zeros((most + 1,), jnp.int32).at[slots].set(source_rows)[:most]
        weights = jnp.zeros((most + 1,), jnp.float32).at[slots].set(jnp.where(mask, flat_weight, 0.0))[:most]
        picked = normed[rows]
        gate = jnp.dot(picked, w_gate[expert].T, preferred_element_type=jnp.float32)
        up = jnp.dot(picked, w_up[expert].T, preferred_element_type=jnp.float32)
        hidden = (jax.nn.silu(gate) * up).astype(jnp.bfloat16)
        expert_out = jnp.dot(hidden, w_down[expert], preferred_element_type=jnp.float32).astype(jnp.bfloat16)
        carry = carry.at[rows].add(expert_out.astype(jnp.float32) * weights[:, None])
        return (carry, None)
    moe, _ = lax.scan(one_expert, jnp.zeros((TOKENS, D), jnp.float32), jnp.arange(EXPERTS, dtype=jnp.int32))
    mixed = moe * lax.rsqrt(lax.optimization_barrier(jnp.mean(moe * moe, axis=1, keepdims=True)) + epsilon) * out_gain.astype(jnp.float32)
    return mixed.astype(jnp.bfloat16)
```

```python
import functools

import jax
import jax.numpy as jnp
from jax import lax
from jax.experimental import pallas as pl
from jax.experimental.pallas import tpu as pltpu
from jax.sharding import PartitionSpec as P

SIDE = 4
CLASSES = 4
EXTRA = 16
epsilon = 1e-06


def klass(i):
    return (i % SIDE + 2 * (i // SIDE)) % CLASSES


def moved(i, dy, dx):
    return (i // SIDE + dy) % SIDE * SIDE + (i % SIDE + dx) % SIDE


def shifted(value, dy, dx):
    n = SIDE * SIDE
    return lax.ppermute(value, "ep", [(i, moved(i, dy, dx)) for i in range(n)])


def slots_of(ids, experts):
    tokens = ids.shape[1]
    expert = lax.broadcasted_iota(jnp.int32, (experts, tokens), 0)
    first, second = ids[0:1] == expert, ids[1:2] == expert
    named = jnp.logical_or(first, second)
    before = lax.broadcasted_iota(jnp.int32, (tokens, tokens), 0) < lax.broadcasted_iota(
        jnp.int32, (tokens, tokens), 1
    )
    rank = jnp.dot(
        named.astype(jnp.float32).astype(jnp.bfloat16),
        before.astype(jnp.float32).astype(jnp.bfloat16),
        preferred_element_type=jnp.float32,
    )
    return first, second, jnp.where(named, rank, -1.0)


def dispatch_kernel(ids_ref, x_ref, out_ref, pick_ref, *, experts, capacity):
    tokens = x_ref.shape[0]
    _, _, slot = slots_of(ids_ref[...], experts)
    place = lax.broadcasted_iota(jnp.int32, (capacity, tokens), 0).astype(jnp.float32)
    for e in range(experts):
        pick = (slot[e : e + 1] == place).astype(jnp.float32).astype(jnp.bfloat16)
        pick_ref[e * capacity : (e + 1) * capacity] = pick
    out_ref[...] = jnp.dot(
        pick_ref[...], x_ref[...], preferred_element_type=jnp.float32
    ).astype(jnp.bfloat16)


def combine_kernel(ids_ref, w_ref, back_ref, moe_ref, sq_ref, pick_ref, *, experts, capacity):
    tokens = ids_ref.shape[1]
    first, second, slot = slots_of(ids_ref[...], experts)
    place = lax.broadcasted_iota(jnp.int32, (capacity, tokens), 0).astype(jnp.float32)
    moe = None
    for k, mine in enumerate((first, second)):
        own = jnp.where(mine, slot, -1.0)
        for e in range(experts):
            pick = (own[e : e + 1] == place).astype(jnp.float32).astype(jnp.bfloat16)
            pick_ref[e * capacity : (e + 1) * capacity] = pick
        picked = lax.dot_general(
            pick_ref[...],
            back_ref[...],
            (((0,), (0,)), ((), ())),
            preferred_element_type=jnp.float32,
        )
        term = picked * w_ref[:, k : k + 1]
        moe = term if moe is None else moe + term
    moe_ref[...] = moe
    squares = lax.dot_general(
        jnp.ones((8, moe.shape[1]), jnp.float32),
        moe * moe,
        (((1,), (1,)), ((), ())),
        precision=lax.Precision.HIGHEST,
        preferred_element_type=jnp.float32,
    )
    for i in range(sq_ref.shape[0]):
        sq_ref[i] = squares[0:1]


def up_kernel(*refs, pieces, width):
    rows_ref = refs[0]
    gates, ups = refs[1 : 1 + pieces], refs[1 + pieces : 1 + 2 * pieces]
    out_ref, x_buf, normed, w_buf, x_sem, w_sem = refs[1 + 2 * pieces :]
    sources, _, local = rows_ref.shape
    units = gates[0].shape[0]
    rows = normed.shape[0]
    x_copies = [
        pltpu.make_async_copy(rows_ref.at[j], x_buf.at[j], x_sem.at[j]) for j in range(sources)
    ]
    w_copies = []
    for n in range(pieces):
        for half, ref in enumerate((gates[n], ups[n])):
            w_copies.append(
                pltpu.make_async_copy(
                    ref, w_buf.at[n, pl.ds(half * units, units)], w_sem.at[n, half]
                )
            )
    for copy in x_copies:
        copy.start()
    for copy in w_copies:
        copy.start()
    squares = jnp.zeros((rows, local), jnp.float32)
    for j in range(sources):
        x_copies[j].wait()
        part = x_buf[j, 0:rows, :].astype(jnp.float32)
        squares = squares + part * part
    scale = lax.rsqrt(jnp.sum(squares, axis=1, keepdims=True) / width + epsilon)
    for j in range(sources):
        gain = x_buf[j, rows : rows + EXTRA, :].astype(jnp.float32)[0:1]
        part = x_buf[j, 0:rows, :].astype(jnp.float32)
        normed[:, j * local : (j + 1) * local] = (part * scale * gain).astype(jnp.bfloat16)
    for n in range(pieces):
        w_copies[2 * n].wait()
        w_copies[2 * n + 1].wait()
        both = lax.dot_general(
            normed[...],
            w_buf[n],
            (((1,), (1,)), ((), ())),
            preferred_element_type=jnp.float32,
        )
        gate, up = both[:, :units], both[:, units:]
        hidden = (gate / (1.0 + jnp.exp(-gate)) * up).astype(jnp.bfloat16)
        for p in range(out_ref.shape[0]):
            out_ref[p, :, n * units : (n + 1) * units] = hidden


def down_kernel(idx_ref, hidden_ref, *refs, pieces):
    weights = refs[:pieces]
    outs = refs[pieces : 2 * pieces]
    h_buf, ordered, w_buf, h_sem, w_sem = refs[2 * pieces :]
    peers = hidden_ref.shape[0]
    units = hidden_ref.shape[2] // pieces
    h_copies = [
        pltpu.make_async_copy(hidden_ref.at[p], h_buf.at[p], h_sem.at[p]) for p in range(peers)
    ]
    w_copies = [
        pltpu.make_async_copy(weights[n], w_buf.at[n], w_sem.at[n]) for n in range(pieces)
    ]
    for copy in h_copies:
        copy.start()
    order = (*range(1, pieces), 0)
    for n in order:
        w_copies[n].start()
    for p in range(peers):
        h_copies[p].wait()
        for n in range(pieces):
            at = pl.multiple_of(idx_ref[p * pieces + n] * units, units)
            ordered[:, pl.ds(at, units)] = h_buf[p, :, n * units : (n + 1) * units]
    for n in order:
        w_copies[n].wait()
        outs[n][...] = jnp.dot(
            ordered[...], w_buf[n], preferred_element_type=jnp.float32
        ).astype(jnp.bfloat16)


def body(tokens, norm_gain, expert_ids, combine_weight, w_gate, w_up, w_down, out_gain):
    tok_rows, local = tokens.shape
    n_split = lax.axis_size("ep")
    n_route = lax.axis_size("tp")
    width = local * n_split
    experts = w_gate.shape[0] * n_route
    capacity = 2 * expert_ids.shape[1] * tok_rows // experts
    slots = experts * capacity
    rows = n_route * capacity // CLASSES
    units = w_gate.shape[1]
    hidden_all = units * n_split
    w_gate, w_up, w_down = w_gate[0], w_up[0], w_down[0]
    vmem = pl.BlockSpec(memory_space=pltpu.VMEM)
    anywhere = pl.BlockSpec(memory_space=pl.ANY)
    ids = expert_ids.T

    buffer = pl.pallas_call(
        functools.partial(dispatch_kernel, experts=experts, capacity=capacity),
        out_shape=jax.ShapeDtypeStruct((slots, local), jnp.bfloat16),
        in_specs=[vmem, vmem],
        out_specs=vmem,
        scratch_shapes=[pltpu.VMEM((slots, tok_rows), jnp.bfloat16)],
        name="dispatch",
    )(ids, tokens)
    arrived = lax.all_to_all(
        buffer.reshape(experts, capacity, local), "tp", split_axis=0, concat_axis=0, tiled=True
    )

    steps = ((0, 1), (0, -1), (1, 0))
    gates = [w_gate, *(shifted(w_gate, *s) for s in steps)]
    ups = [w_up, *(shifted(w_up, *s) for s in steps)]
    downs = [w_down, *(shifted(w_down, *s) for s in steps)]
    pieces = len(gates)

    quarters = arrived.reshape(CLASSES, rows, local)
    gain_rows = jnp.broadcast_to(norm_gain[None, :], (EXTRA, local))
    parts = [jnp.concatenate([quarters[q], gain_rows], axis=0) for q in range(CLASSES)]
    operand = jnp.stack([parts[klass(i)] for i in range(n_split)])
    gathered = lax.all_to_all(operand, "ep", split_axis=0, concat_axis=0, tiled=True)

    hidden = pl.pallas_call(
        functools.partial(up_kernel, pieces=pieces, width=width),
        out_shape=jax.ShapeDtypeStruct((SIDE, rows, pieces * units), jnp.bfloat16),
        in_specs=[anywhere] * (1 + 2 * pieces),
        out_specs=vmem,
        scratch_shapes=[
            pltpu.VMEM((n_split, rows + EXTRA, local), jnp.bfloat16),
            pltpu.VMEM((rows, width), jnp.bfloat16),
            pltpu.VMEM((pieces, 2 * units, width), jnp.bfloat16),
            pltpu.SemaphoreType.DMA((n_split,)),
            pltpu.SemaphoreType.DMA((pieces, 2)),
        ],
        name="gate_up",
    )(gathered, *gates, *ups)

    groups = [[i for i in range(n_split) if klass(i) == q] for q in range(CLASSES)]
    shared = lax.all_to_all(
        hidden, "ep", split_axis=0, concat_axis=0, tiled=True, axis_index_groups=groups
    )
    me = lax.axis_index("ep")
    mine = klass(me)
    table = jnp.asarray(
        [
            [[i, *(moved(i, -dy, -dx) for dy, dx in steps)] for i in group]
            for group in groups
        ],
        jnp.int32,
    ).reshape(CLASSES, SIDE * pieces)
    order = lax.dynamic_index_in_dim(table, mine, 0, keepdims=False)

    outs = pl.pallas_call(
        functools.partial(down_kernel, pieces=pieces),
        out_shape=[jax.ShapeDtypeStruct((rows, local), jnp.bfloat16)] * pieces,
        in_specs=[pl.BlockSpec(memory_space=pltpu.SMEM)] + [anywhere] * (1 + pieces),
        out_specs=[vmem] * pieces,
        scratch_shapes=[
            pltpu.VMEM((SIDE, rows, pieces * units), jnp.bfloat16),
            pltpu.VMEM((rows, hidden_all), jnp.bfloat16),
            pltpu.VMEM((pieces, hidden_all, local), jnp.bfloat16),
            pltpu.SemaphoreType.DMA((SIDE,)),
            pltpu.SemaphoreType.DMA((pieces,)),
        ],
        name="down",
    )(order, shared, *downs)

    returned = jnp.zeros((CLASSES, rows, local), jnp.bfloat16)
    for out, (dy, dx) in zip(outs[1:], steps):
        back = shifted(out, -dy, -dx)
        q = (mine + dx + 2 * dy) % CLASSES
        returned = lax.dynamic_update_index_in_dim(returned, back, q, 0)
    returned = lax.dynamic_update_index_in_dim(returned, outs[0], mine, 0)

    answers = lax.all_to_all(
        returned.reshape(n_route, capacity, local), "tp", split_axis=0, concat_axis=0, tiled=True
    )
    moe, squares = pl.pallas_call(
        functools.partial(combine_kernel, experts=experts, capacity=capacity),
        out_shape=[
            jax.ShapeDtypeStruct((tok_rows, local), jnp.float32),
            jax.ShapeDtypeStruct((n_split, 1, tok_rows), jnp.float32),
        ],
        in_specs=[vmem] * 3,
        out_specs=[vmem] * 2,
        scratch_shapes=[pltpu.VMEM((slots, tok_rows), jnp.bfloat16)],
        name="combine",
    )(ids, combine_weight, answers.reshape(slots, local))
    squares = lax.all_to_all(squares, "ep", split_axis=0, concat_axis=0, tiled=True)
    total = jnp.sum(squares, axis=(0, 1))
    mixed = (
        moe * lax.rsqrt(total / width + epsilon)[:, None] * out_gain.astype(jnp.float32)[None, :]
    )
    return mixed.astype(jnp.bfloat16)


def solution(mesh):
    return jax.shard_map(
        body,
        mesh=mesh,
        in_specs=(
            P("tp", "ep"),
            P("ep"),
            P("tp", None),
            P("tp", None),
            P("tp", "ep", None),
            P("tp", "ep", None),
            P("tp", None, "ep"),
            P("ep"),
        ),
        out_specs=P("tp", "ep"),
        check_vma=False,
    )
```

```python
import functools

import jax
import jax.numpy as jnp
from jax import lax
from jax.experimental import pallas as pl
from jax.experimental.pallas import tpu as pltpu
from jax.sharding import PartitionSpec as P


SIDE = 4
CLASSES = 4
EXTRA = 16
epsilon = 1e-06


GRANT = 24 * 1024 * 1024


def klass(i):
    return (i % SIDE + 2 * (i // SIDE)) % CLASSES


def moved(i, dy, dx):
    return (i // SIDE + dy) % SIDE * SIDE + (i % SIDE + dx) % SIDE


def shifted(value, dy, dx):
    n = SIDE * SIDE
    return lax.ppermute(value, "ep", [(i, moved(i, dy, dx)) for i in range(n)])


def slots_of(ids, experts):
    tokens = ids.shape[1]
    expert = lax.broadcasted_iota(jnp.int32, (experts, tokens), 0)
    first, second = ids[0:1] == expert, ids[1:2] == expert
    named = jnp.logical_or(first, second)
    before = lax.broadcasted_iota(jnp.int32, (tokens, tokens), 0) < lax.broadcasted_iota(
        jnp.int32, (tokens, tokens), 1
    )
    rank = jnp.dot(
        named.astype(jnp.float32).astype(jnp.bfloat16),
        before.astype(jnp.float32).astype(jnp.bfloat16),
        preferred_element_type=jnp.float32,
    )
    return first, second, jnp.where(named, rank, -1.0)


def dispatch_kernel(ids_ref, x_ref, out_ref, pick_ref, *, experts, capacity):
    tokens = x_ref.shape[0]
    _, _, slot = slots_of(ids_ref[...], experts)
    place = lax.broadcasted_iota(jnp.int32, (capacity, tokens), 0).astype(jnp.float32)
    for e in range(experts):
        pick = (slot[e : e + 1] == place).astype(jnp.float32).astype(jnp.bfloat16)
        pick_ref[e * capacity : (e + 1) * capacity] = pick
    out_ref[...] = jnp.dot(
        pick_ref[...], x_ref[...], preferred_element_type=jnp.float32
    ).astype(jnp.bfloat16)


def prepare_kernel(ids_ref, w_ref, pick_ref, out_ref, *, experts, capacity):
    tokens = ids_ref.shape[1]
    first, second, slot = slots_of(ids_ref[...], experts)
    place = lax.broadcasted_iota(jnp.int32, (capacity, tokens), 0).astype(jnp.float32)
    for k, mine in enumerate((first, second)):
        own = jnp.where(mine, slot, -1.0)
        for e in range(experts):
            pick = (own[e : e + 1] == place).astype(jnp.float32).astype(jnp.bfloat16)
            pick_ref[k, e * capacity : (e + 1) * capacity] = pick
    for k in range(w_ref.shape[0]):
        out_ref[k] = jnp.broadcast_to(w_ref[k : k + 1], out_ref.shape[1:][::-1]).T


def combine_kernel(pick_ref, w_ref, back_ref, moe_ref, sq_ref):
    moe = None
    for k in range(w_ref.shape[0]):
        picked = lax.dot_general(
            pick_ref[k],
            back_ref[...],
            (((0,), (0,)), ((), ())),
            preferred_element_type=jnp.float32,
        )
        term = picked * w_ref[k][:, 0:1]
        moe = term if moe is None else moe + term
    moe_ref[...] = moe
    squares = lax.dot_general(
        jnp.ones((8, moe.shape[1]), jnp.float32),
        moe * moe,
        (((1,), (1,)), ((), ())),
        precision=lax.Precision.HIGHEST,
        preferred_element_type=jnp.float32,
    )
    for i in range(sq_ref.shape[0]):
        sq_ref[i] = squares[0:1]


def spread_kernel(rows_ref, gain_ref, out_ref):
    rows = rows_ref.shape[1]
    gain = jnp.broadcast_to(gain_ref[...].astype(jnp.float32), (EXTRA, rows_ref.shape[2]))
    gain = gain.astype(jnp.bfloat16)
    for i in range(out_ref.shape[0]):
        out_ref[i, 0:rows, :] = rows_ref[klass(i)]
        out_ref[i, rows : rows + EXTRA, :] = gain


def up_kernel(*refs, pieces, width):
    rows_ref = refs[0]
    gates, ups = refs[1 : 1 + pieces], refs[1 + pieces : 1 + 2 * pieces]
    out_ref, normed = refs[1 + 2 * pieces :]
    sources, _, local = rows_ref.shape
    units = gates[0].shape[0]
    rows = normed.shape[0]
    squares = jnp.zeros((rows, local), jnp.float32)
    for j in range(sources):
        part = rows_ref[j, 0:rows, :].astype(jnp.float32)
        squares = squares + part * part
    scale = lax.rsqrt(jnp.sum(squares, axis=1, keepdims=True) / width + epsilon)
    for j in range(sources):
        gain = rows_ref[j, rows : rows + EXTRA, :].astype(jnp.float32)[0:1]
        part = rows_ref[j, 0:rows, :].astype(jnp.float32)
        normed[:, j * local : (j + 1) * local] = (part * scale * gain).astype(jnp.bfloat16)
    for n in range(pieces):
        both = lax.dot_general(
            normed[...],
            jnp.concatenate([gates[n][...], ups[n][...]], axis=0),
            (((1,), (1,)), ((), ())),
            preferred_element_type=jnp.float32,
        )
        gate, up = both[:, :units], both[:, units:]
        hidden = (gate / (1.0 + jnp.exp(-gate)) * up).astype(jnp.bfloat16)
        for p in range(out_ref.shape[0]):
            out_ref[p, :, n * units : (n + 1) * units] = hidden


def down_kernel(idx_ref, hidden_ref, *refs, pieces):
    weights = refs[:pieces]
    outs = refs[pieces : 2 * pieces]
    ordered = refs[2 * pieces]
    units = hidden_ref.shape[2] // pieces
    for p in range(hidden_ref.shape[0]):
        for n in range(pieces):
            at = pl.multiple_of(idx_ref[p * pieces + n] * units, units)
            ordered[:, pl.ds(at, units)] = hidden_ref[p, :, n * units : (n + 1) * units]
    for n in range(pieces):
        outs[n][...] = jnp.dot(
            ordered[...], weights[n][...], preferred_element_type=jnp.float32
        ).astype(jnp.bfloat16)


def gather_kernel(q_ref, *refs):
    out_ref = refs[-1]
    for i, ref in enumerate(refs[:-1]):
        out_ref[q_ref[i]] = ref[...]


def in_vmem(value):
    return pltpu.with_memory_space_constraint(value, pltpu.VMEM)


def body(tokens, norm_gain, expert_ids, combine_weight, w_gate, w_up, w_down, out_gain):
    tok_rows, local = tokens.shape
    n_split = lax.axis_size("ep")
    n_route = lax.axis_size("tp")
    width = local * n_split
    experts = w_gate.shape[0] * n_route
    capacity = 2 * expert_ids.shape[1] * tok_rows // experts
    slots = experts * capacity
    rows = n_route * capacity // CLASSES
    units = w_gate.shape[1]
    hidden_all = units * n_split
    w_gate, w_up, w_down = w_gate[0], w_up[0], w_down[0]
    vmem = pl.BlockSpec(memory_space=pltpu.VMEM)
    ids = expert_ids.T

    buffer = pl.pallas_call(
        functools.partial(dispatch_kernel, experts=experts, capacity=capacity),
        out_shape=pltpu.VMEM((slots, local), jnp.bfloat16),
        in_specs=[vmem, vmem],
        out_specs=vmem,
        scratch_shapes=[pltpu.VMEM((slots, tok_rows), jnp.bfloat16)],
        compiler_params=pltpu.CompilerParams(vmem_limit_bytes=GRANT),
        name="dispatch",
    )(ids, tokens)
    arrived = lax.all_to_all(
        buffer.reshape(experts, capacity, local),
        "tp",
        split_axis=0,
        concat_axis=0,
        tiled=True,
    )

    steps = ((0, 1), (0, -1), (1, 0))
    gates = [w_gate, *(shifted(w_gate, *s) for s in steps)]
    ups = [w_up, *(shifted(w_up, *s) for s in steps)]
    downs = [w_down, *(shifted(w_down, *s) for s in steps)]
    pieces = len(gates)

    picks, weights = pl.pallas_call(
        functools.partial(prepare_kernel, experts=experts, capacity=capacity),
        out_shape=[
            pltpu.VMEM((expert_ids.shape[1], slots, tok_rows), jnp.bfloat16),
            pltpu.VMEM((expert_ids.shape[1], tok_rows, 128), jnp.float32),
        ],
        in_specs=[vmem, vmem],
        out_specs=[vmem, vmem],
        compiler_params=pltpu.CompilerParams(vmem_limit_bytes=GRANT),
        name="prepare",
    )(ids, combine_weight.T)
    operand = pl.pallas_call(
        spread_kernel,
        out_shape=pltpu.VMEM((n_split, rows + EXTRA, local), jnp.bfloat16),
        in_specs=[vmem, vmem],
        out_specs=vmem,
        compiler_params=pltpu.CompilerParams(vmem_limit_bytes=GRANT),
        name="spread",
    )(in_vmem(arrived.reshape(CLASSES, rows, local)), norm_gain[None, :])
    gathered = lax.all_to_all(operand, "ep", split_axis=0, concat_axis=0, tiled=True)

    hidden = pl.pallas_call(
        functools.partial(up_kernel, pieces=pieces, width=width),
        out_shape=pltpu.VMEM((SIDE, rows, pieces * units), jnp.bfloat16),
        in_specs=[vmem] * (1 + 2 * pieces),
        out_specs=vmem,
        scratch_shapes=[pltpu.VMEM((rows, width), jnp.bfloat16)],
        compiler_params=pltpu.CompilerParams(vmem_limit_bytes=GRANT),
        name="gate_up",
    )(in_vmem(gathered), *(in_vmem(w) for w in (*gates, *ups)))

    groups = [[i for i in range(n_split) if klass(i) == q] for q in range(CLASSES)]
    shared = lax.all_to_all(
        hidden, "ep", split_axis=0, concat_axis=0, tiled=True, axis_index_groups=groups
    )
    mine = klass(lax.axis_index("ep"))
    table = jnp.asarray(
        [
            [[i, *(moved(i, -dy, -dx) for dy, dx in steps)] for i in group]
            for group in groups
        ],
        jnp.int32,
    ).reshape(CLASSES, SIDE * pieces)
    order = lax.dynamic_index_in_dim(table, mine, 0, keepdims=False)

    outs = pl.pallas_call(
        functools.partial(down_kernel, pieces=pieces),
        out_shape=[pltpu.VMEM((rows, local), jnp.bfloat16)] * pieces,
        in_specs=[pl.BlockSpec(memory_space=pltpu.SMEM)] + [vmem] * (1 + pieces),
        out_specs=[vmem] * pieces,
        scratch_shapes=[pltpu.VMEM((rows, hidden_all), jnp.bfloat16)],
        compiler_params=pltpu.CompilerParams(vmem_limit_bytes=GRANT),
        name="down",
    )(order, in_vmem(shared), *(in_vmem(w) for w in downs))

    pieces_back = [outs[0], *(shifted(out, -dy, -dx) for out, (dy, dx) in zip(outs[1:], steps))]
    places = jnp.asarray([0, *(dx + 2 * dy for dy, dx in steps)], jnp.int32)
    places = (mine + places) % CLASSES
    returned = pl.pallas_call(
        gather_kernel,
        out_shape=pltpu.VMEM((CLASSES, rows, local), jnp.bfloat16),
        in_specs=[pl.BlockSpec(memory_space=pltpu.SMEM)] + [vmem] * pieces,
        out_specs=vmem,
        compiler_params=pltpu.CompilerParams(vmem_limit_bytes=GRANT),
        name="gather",
    )(places, *(in_vmem(piece) for piece in pieces_back))

    answers = lax.all_to_all(
        returned.reshape(n_route, capacity, local),
        "tp",
        split_axis=0,
        concat_axis=0,
        tiled=True,
    )
    moe, squares = pl.pallas_call(
        combine_kernel,
        out_shape=[
            pltpu.VMEM((tok_rows, local), jnp.float32),
            pltpu.VMEM((n_split, 1, tok_rows), jnp.float32),
        ],
        in_specs=[vmem] * 3,
        out_specs=[vmem] * 2,
        compiler_params=pltpu.CompilerParams(vmem_limit_bytes=GRANT),
        name="combine",
    )(in_vmem(picks), in_vmem(weights), in_vmem(answers.reshape(slots, local)))
    squares = lax.all_to_all(squares, "ep", split_axis=0, concat_axis=0, tiled=True)
    total = jnp.sum(squares, axis=(0, 1))
    mixed = (
        moe
        * lax.rsqrt(total / width + epsilon)[:, None]
        * out_gain.astype(jnp.float32)[None, :]
    )
    return mixed.astype(jnp.bfloat16)


def solution(mesh):
    return jax.shard_map(
        body,
        mesh=mesh,
        in_specs=(
            P("tp", "ep"),
            P("ep"),
            P("tp", None),
            P("tp", None),
            P("tp", "ep", None),
            P("tp", "ep", None),
            P("tp", None, "ep"),
            P("ep"),
        ),
        out_specs=P("tp", "ep"),
        check_vma=False,
    )
```

```python
import functools

import jax
import jax.numpy as jnp
from jax import lax
from jax.experimental import pallas as pl
from jax.experimental.pallas import tpu as pltpu
from jax.sharding import PartitionSpec as P


SIDE = 4
CLASSES = 4
EXTRA = 16
epsilon = 1e-06


GRANT = 24 * 1024 * 1024


def turn(i, core):
    return i if core == 0 else i % SIDE * SIDE + i // SIDE


def klass(i):
    return (i % SIDE + 2 * (i // SIDE)) % CLASSES


def moved(i, dy, dx):
    return (i // SIDE + dy) % SIDE * SIDE + (i % SIDE + dx) % SIDE


def shifted(value, dy, dx):
    n_route = lax.axis_size("tp")
    pairs = []
    for i in range(SIDE * SIDE):
        for t in range(n_route):
            to = turn(moved(turn(i, t % 2), dy, dx), t % 2)
            pairs.append((i * n_route + t, to * n_route + t))
    return lax.ppermute(value, ("ep", "tp"), pairs)


def spread_weights(weight, steps):
    half = weight.shape[0] // 2
    return [
        weight,
        *(shifted(weight, *s) for s in steps),
        shifted(weight[:half], -1, 0),
        shifted(weight[half:], 1, 0),
    ]


def slots_of(ids, experts):
    tokens = ids.shape[1]
    expert = lax.broadcasted_iota(jnp.int32, (experts, tokens), 0)
    first, second = ids[0:1] == expert, ids[1:2] == expert
    named = jnp.logical_or(first, second)
    before = lax.broadcasted_iota(jnp.int32, (tokens, tokens), 0) < lax.broadcasted_iota(
        jnp.int32, (tokens, tokens), 1
    )
    rank = jnp.dot(
        named.astype(jnp.float32).astype(jnp.bfloat16),
        before.astype(jnp.float32).astype(jnp.bfloat16),
        preferred_element_type=jnp.float32,
    )
    return first, second, jnp.where(named, rank, -1.0)


def dispatch_kernel(ids_ref, x_ref, out_ref, pick_ref, *, experts, capacity):
    tokens = x_ref.shape[0]
    _, _, slot = slots_of(ids_ref[...], experts)
    place = lax.broadcasted_iota(jnp.int32, (capacity, tokens), 0).astype(jnp.float32)
    for e in range(experts):
        pick = (slot[e : e + 1] == place).astype(jnp.float32).astype(jnp.bfloat16)
        pick_ref[e * capacity : (e + 1) * capacity] = pick
    out_ref[...] = jnp.dot(
        pick_ref[...], x_ref[...], preferred_element_type=jnp.float32
    ).astype(jnp.bfloat16)


def prepare_kernel(ids_ref, w_ref, pick_ref, out_ref, *, experts, capacity):
    tokens = ids_ref.shape[1]
    first, second, slot = slots_of(ids_ref[...], experts)
    place = lax.broadcasted_iota(jnp.int32, (capacity, tokens), 0).astype(jnp.float32)
    for k, mine in enumerate((first, second)):
        own = jnp.where(mine, slot, -1.0)
        for e in range(experts):
            pick = (own[e : e + 1] == place).astype(jnp.float32).astype(jnp.bfloat16)
            pick_ref[k, e * capacity : (e + 1) * capacity] = pick
    for k in range(w_ref.shape[0]):
        out_ref[k] = jnp.broadcast_to(w_ref[k : k + 1], out_ref.shape[1:][::-1]).T


def combine_kernel(pick_ref, w_ref, back_ref, moe_ref, sq_ref):
    moe = None
    for k in range(w_ref.shape[0]):
        picked = lax.dot_general(
            pick_ref[k],
            back_ref[...],
            (((0,), (0,)), ((), ())),
            preferred_element_type=jnp.float32,
        )
        term = picked * w_ref[k][:, 0:1]
        moe = term if moe is None else moe + term
    moe_ref[...] = moe
    squares = lax.dot_general(
        jnp.ones((8, moe.shape[1]), jnp.float32),
        moe * moe,
        (((1,), (1,)), ((), ())),
        precision=lax.Precision.HIGHEST,
        preferred_element_type=jnp.float32,
    )
    for i in range(sq_ref.shape[0]):
        sq_ref[i] = squares[0:1]


def spread_kernel(q_ref, rows_ref, gain_ref, out_ref):
    rows = rows_ref.shape[1]
    gain = jnp.broadcast_to(gain_ref[...].astype(jnp.float32), (EXTRA, rows_ref.shape[2]))
    gain = gain.astype(jnp.bfloat16)
    for i in range(out_ref.shape[0]):
        out_ref[i, 0:rows, :] = rows_ref[q_ref[i]]
        out_ref[i, rows : rows + EXTRA, :] = gain


def up_kernel(*refs, given, width):
    rows_ref = refs[0]
    gates, ups = refs[1 : 1 + given], refs[1 + given : 1 + 2 * given]
    out_ref, normed = refs[1 + 2 * given :]
    sources, _, local = rows_ref.shape
    units = gates[0].shape[0]
    rows = normed.shape[0]
    squares = jnp.zeros((rows, local), jnp.float32)
    for j in range(sources):
        part = rows_ref[j, 0:rows, :].astype(jnp.float32)
        squares = squares + part * part
    scale = lax.rsqrt(jnp.sum(squares, axis=1, keepdims=True) / width + epsilon)
    for j in range(sources):
        gain = rows_ref[j, rows : rows + EXTRA, :].astype(jnp.float32)[0:1]
        part = rows_ref[j, 0:rows, :].astype(jnp.float32)
        normed[:, j * local : (j + 1) * local] = (part * scale * gain).astype(jnp.bfloat16)
    for n in range(given - 1):
        last = given if n == given - 2 else n + 1
        both = lax.dot_general(
            normed[...],
            jnp.concatenate([ref[...] for ref in (*gates[n:last], *ups[n:last])], axis=0),
            (((1,), (1,)), ((), ())),
            preferred_element_type=jnp.float32,
        )
        gate, up = both[:, :units], both[:, units:]
        hidden = (gate / (1.0 + jnp.exp(-gate)) * up).astype(jnp.bfloat16)
        for p in range(out_ref.shape[0]):
            out_ref[p, :, n * units : (n + 1) * units] = hidden


def down_kernel(idx_ref, hidden_ref, *refs, pieces):
    weights = refs[:pieces]
    outs = refs[pieces : 2 * pieces]
    ordered = refs[2 * pieces]
    units = hidden_ref.shape[2] // pieces
    for p in range(hidden_ref.shape[0]):
        for n in range(pieces):
            at = pl.multiple_of(idx_ref[p * pieces + n] * units, units)
            part = hidden_ref[p, :, n * units : (n + 1) * units]
            if n == pieces - 1:
                other = hidden_ref[p ^ 2, :, n * units : (n + 1) * units]
                lane = lax.broadcasted_iota(jnp.int32, part.shape, 1)
                part = jnp.where(
                    lane < units // 2, part.astype(jnp.float32), other.astype(jnp.float32)
                ).astype(jnp.bfloat16)
            ordered[:, pl.ds(at, units)] = part
    for n in range(pieces):
        outs[n][...] = jnp.dot(
            ordered[...], weights[n][...], preferred_element_type=jnp.float32
        ).astype(jnp.bfloat16)


def gather_kernel(q_ref, *refs):
    out_ref = refs[-1]
    for i, ref in enumerate(refs[:-1]):
        out_ref[q_ref[i]] = ref[...]


def in_vmem(value):
    return pltpu.with_memory_space_constraint(value, pltpu.VMEM)


def body(tokens, norm_gain, expert_ids, combine_weight, w_gate, w_up, w_down, out_gain):
    tok_rows, local = tokens.shape
    n_split = lax.axis_size("ep")
    n_route = lax.axis_size("tp")
    width = local * n_split
    experts = w_gate.shape[0] * n_route
    capacity = 2 * expert_ids.shape[1] * tok_rows // experts
    slots = experts * capacity
    rows = n_route * capacity // CLASSES
    units = w_gate.shape[1]
    hidden_all = units * n_split
    w_gate, w_up, w_down = w_gate[0], w_up[0], w_down[0]
    vmem = pl.BlockSpec(memory_space=pltpu.VMEM)
    ids = expert_ids.T

    smem = pl.BlockSpec(memory_space=pltpu.SMEM)
    core = lax.axis_index("tp") % 2
    me = lax.axis_index("ep")
    place = jnp.where(core == 0, me, turn(me, 1))
    mine = klass(place)
    class_of = jnp.asarray(
        [[klass(turn(i, k)) for i in range(n_split)] for k in range(2)], jnp.int32
    )
    class_of = lax.dynamic_index_in_dim(class_of, core, 0, keepdims=False)
    buffer = pl.pallas_call(
        functools.partial(dispatch_kernel, experts=experts, capacity=capacity),
        out_shape=jax.ShapeDtypeStruct((slots, local), jnp.bfloat16),
        in_specs=[vmem, vmem],
        out_specs=vmem,
        scratch_shapes=[pltpu.VMEM((slots, tok_rows), jnp.bfloat16)],
        compiler_params=pltpu.CompilerParams(vmem_limit_bytes=GRANT),
        name="dispatch",
    )(ids, tokens)
    arrived = lax.all_to_all(
        buffer.reshape(experts, capacity, local),
        "tp",
        split_axis=0,
        concat_axis=0,
        tiled=True,
    )

    steps = ((0, 1), (0, -1))
    last_steps = ((0, 1), (0, -1), (1, 0))
    gates = spread_weights(w_gate, steps)
    ups = spread_weights(w_up, steps)
    downs = [w_down, *(shifted(w_down, *s) for s in last_steps)]
    given, pieces = len(gates), len(downs)

    picks, weights = pl.pallas_call(
        functools.partial(prepare_kernel, experts=experts, capacity=capacity),
        out_shape=[
            pltpu.VMEM((expert_ids.shape[1], slots, tok_rows), jnp.bfloat16),
            pltpu.VMEM((expert_ids.shape[1], tok_rows, 128), jnp.float32),
        ],
        in_specs=[vmem, vmem],
        out_specs=[vmem, vmem],
        compiler_params=pltpu.CompilerParams(vmem_limit_bytes=GRANT),
        name="prepare",
    )(ids, combine_weight.T)
    operand = pl.pallas_call(
        spread_kernel,
        out_shape=jax.ShapeDtypeStruct((n_split, rows + EXTRA, local), jnp.bfloat16),
        in_specs=[smem, vmem, vmem],
        out_specs=vmem,
        compiler_params=pltpu.CompilerParams(vmem_limit_bytes=GRANT),
        name="spread",
    )(class_of, in_vmem(arrived.reshape(CLASSES, rows, local)), norm_gain[None, :])
    gathered = lax.all_to_all(operand, "ep", split_axis=0, concat_axis=0, tiled=True)

    hidden = pl.pallas_call(
        functools.partial(up_kernel, given=given, width=width),
        out_shape=jax.ShapeDtypeStruct((SIDE, rows, pieces * units), jnp.bfloat16),
        in_specs=[vmem] * (1 + 2 * given),
        out_specs=vmem,
        scratch_shapes=[pltpu.VMEM((rows, width), jnp.bfloat16)],
        compiler_params=pltpu.CompilerParams(vmem_limit_bytes=GRANT),
        name="gate_up",
    )(in_vmem(gathered), *(in_vmem(w) for w in (*gates, *ups)))

    groups = [
        [
            [turn(v, k) for v in range(n_split) if klass(v) == q]
            for q in range(CLASSES)
        ]
        for k in range(2)
    ]
    shared = lax.all_to_all(
        hidden,
        ("ep", "tp"),
        split_axis=0,
        concat_axis=0,
        tiled=True,
        axis_index_groups=[
            [i * n_route + t for i in group]
            for t in range(n_route)
            for group in groups[t % 2]
        ],
    )
    table = jnp.asarray(
        [
            [
                [
                    turn(v, k)
                    for i in group
                    for v in (
                        turn(i, k),
                        *(moved(turn(i, k), -dy, -dx) for dy, dx in steps),
                        moved(turn(i, k), 1, 0),
                    )
                ]
                for group in groups[k]
            ]
            for k in range(2)
        ],
        jnp.int32,
    ).reshape(2 * CLASSES, SIDE * pieces)
    order = lax.dynamic_index_in_dim(table, core * CLASSES + mine, 0, keepdims=False)

    outs = pl.pallas_call(
        functools.partial(down_kernel, pieces=pieces),
        out_shape=[pltpu.VMEM((rows, local), jnp.bfloat16)] * pieces,
        in_specs=[smem] + [vmem] * (1 + pieces),
        out_specs=[vmem] * pieces,
        scratch_shapes=[pltpu.VMEM((rows, hidden_all), jnp.bfloat16)],
        compiler_params=pltpu.CompilerParams(vmem_limit_bytes=GRANT),
        name="down",
    )(order, in_vmem(shared), *(in_vmem(w) for w in downs))

    pieces_back = [
        outs[0],
        *(shifted(out, -dy, -dx) for out, (dy, dx) in zip(outs[1:], last_steps)),
    ]
    places = jnp.asarray([0, *(dx + 2 * dy for dy, dx in last_steps)], jnp.int32)
    places = (mine + places) % CLASSES
    returned = pl.pallas_call(
        gather_kernel,
        out_shape=pltpu.VMEM((CLASSES, rows, local), jnp.bfloat16),
        in_specs=[smem] + [vmem] * pieces,
        out_specs=vmem,
        compiler_params=pltpu.CompilerParams(vmem_limit_bytes=GRANT),
        name="gather",
    )(places, *(in_vmem(piece) for piece in pieces_back))

    answers = lax.all_to_all(
        returned.reshape(n_route, capacity, local),
        "tp",
        split_axis=0,
        concat_axis=0,
        tiled=True,
    )
    moe, squares = pl.pallas_call(
        combine_kernel,
        out_shape=[
            pltpu.VMEM((tok_rows, local), jnp.float32),
            pltpu.VMEM((n_split, 1, tok_rows), jnp.float32),
        ],
        in_specs=[vmem] * 3,
        out_specs=[vmem] * 2,
        compiler_params=pltpu.CompilerParams(vmem_limit_bytes=GRANT),
        name="combine",
    )(in_vmem(picks), in_vmem(weights), in_vmem(answers.reshape(slots, local)))
    squares = lax.all_to_all(squares, "ep", split_axis=0, concat_axis=0, tiled=True)
    total = jnp.sum(squares, axis=(0, 1))
    mixed = (
        moe
        * lax.rsqrt(total / width + epsilon)[:, None]
        * out_gain.astype(jnp.float32)[None, :]
    )
    return mixed.astype(jnp.bfloat16)


def solution(mesh):
    return jax.shard_map(
        body,
        mesh=mesh,
        in_specs=(
            P("tp", "ep"),
            P("ep"),
            P("tp", None),
            P("tp", None),
            P("tp", "ep", None),
            P("tp", "ep", None),
            P("tp", None, "ep"),
            P("ep"),
        ),
        out_specs=P("tp", "ep"),
        check_vma=False,
    )
```

```python
import functools

import jax
import jax.numpy as jnp
from jax import lax
from jax.experimental import pallas as pl
from jax.experimental.pallas import tpu as pltpu
from jax.sharding import PartitionSpec as P


SIDE = 4
CLASSES = 4
EXTRA = 16
epsilon = 1e-06


GRANT = 24 * 1024 * 1024


def turn(i, core):
    return i if core == 0 else i % SIDE * SIDE + i // SIDE


def klass(i):
    return (i % SIDE + 2 * (i // SIDE)) % CLASSES


def moved(i, dy, dx):
    return (i // SIDE + dy) % SIDE * SIDE + (i % SIDE + dx) % SIDE


def shifted(value, dy, dx):
    n_route = lax.axis_size("tp")
    pairs = []
    for i in range(SIDE * SIDE):
        for t in range(n_route):
            to = turn(moved(turn(i, t % 2), dy, dx), t % 2)
            pairs.append((i * n_route + t, to * n_route + t))
    return lax.ppermute(value, ("ep", "tp"), pairs)


def spread_weights(weight, steps):
    half = weight.shape[0] // 2
    return [
        weight,
        *(shifted(weight, *s) for s in steps),
        shifted(weight[:half], -1, 0),
        shifted(weight[half:], 1, 0),
    ]


def slots_of(ids, experts):
    tokens = ids.shape[1]
    expert = lax.broadcasted_iota(jnp.int32, (experts, tokens), 0)
    first, second = ids[0:1] == expert, ids[1:2] == expert
    named = jnp.logical_or(first, second)
    before = lax.broadcasted_iota(jnp.int32, (tokens, tokens), 0) < lax.broadcasted_iota(
        jnp.int32, (tokens, tokens), 1
    )
    rank = jnp.dot(
        named.astype(jnp.float32).astype(jnp.bfloat16),
        before.astype(jnp.float32).astype(jnp.bfloat16),
        preferred_element_type=jnp.float32,
    )
    return first, second, jnp.where(named, rank, -1.0)


def dispatch_kernel(ids_ref, x_ref, out_ref, pick_ref, *, experts, capacity):
    tokens = x_ref.shape[0]
    _, _, slot = slots_of(ids_ref[...], experts)
    place = lax.broadcasted_iota(jnp.int32, (capacity, tokens), 0).astype(jnp.float32)
    for e in range(experts):
        pick = (slot[e : e + 1] == place).astype(jnp.float32).astype(jnp.bfloat16)
        pick_ref[e * capacity : (e + 1) * capacity] = pick
    out_ref[...] = jnp.dot(
        pick_ref[...], x_ref[...], preferred_element_type=jnp.float32
    ).astype(jnp.bfloat16)


def prepare_kernel(ids_ref, w_ref, pick_ref, out_ref, *, experts, capacity):
    first, second, slot = slots_of(ids_ref[...], experts)
    tall = out_ref.shape[1:][::-1]
    base = lax.broadcasted_iota(jnp.int32, slot.shape, 0).astype(jnp.float32) * capacity
    place = lax.broadcasted_iota(jnp.int32, pick_ref.shape[1:], 1).astype(jnp.float32)
    for k, mine in enumerate((first, second)):
        target = jnp.sum(jnp.where(mine, base + slot, 0.0), axis=0, keepdims=True)
        target = jnp.broadcast_to(target, tall).T[:, 0:1]
        pick_ref[k] = (place == target).astype(jnp.float32).astype(jnp.bfloat16)
    for k in range(w_ref.shape[0]):
        out_ref[k] = jnp.broadcast_to(w_ref[k : k + 1], tall).T


def combine_kernel(pick_ref, w_ref, back_ref, moe_ref, sq_ref):
    routes, tokens, slots = pick_ref.shape
    picked = jnp.dot(
        pick_ref[...].reshape(routes * tokens, slots),
        back_ref[...],
        preferred_element_type=jnp.float32,
    )
    moe = None
    for k in range(routes):
        term = picked[k * tokens : (k + 1) * tokens] * w_ref[k][:, 0:1]
        moe = term if moe is None else moe + term
    moe_ref[...] = moe
    squares = jnp.sum(moe * moe, axis=1, keepdims=True)
    squares = jnp.broadcast_to(squares, (tokens, 128)).T
    for i in range(sq_ref.shape[0]):
        sq_ref[i] = squares[0:1]


def spread_kernel(q_ref, rows_ref, gain_ref, out_ref):
    rows = rows_ref.shape[1]
    gain = jnp.broadcast_to(gain_ref[...].astype(jnp.float32), (EXTRA, rows_ref.shape[2]))
    gain = gain.astype(jnp.bfloat16)
    for i in range(out_ref.shape[0]):
        out_ref[i, 0:rows, :] = rows_ref[q_ref[i]]
        out_ref[i, rows : rows + EXTRA, :] = gain


def up_kernel(*refs, given, width):
    rows_ref = refs[0]
    gates, ups = refs[1 : 1 + given], refs[1 + given : 1 + 2 * given]
    out_ref, normed = refs[1 + 2 * given :]
    sources, _, local = rows_ref.shape
    units = gates[0].shape[0]
    rows = normed.shape[0]
    squares = jnp.zeros((rows, local), jnp.float32)
    for j in range(sources):
        part = rows_ref[j, 0:rows, :].astype(jnp.float32)
        squares = squares + part * part
    scale = lax.rsqrt(jnp.sum(squares, axis=1, keepdims=True) / width + epsilon)
    for j in range(sources):
        gain = rows_ref[j, rows : rows + EXTRA, :].astype(jnp.float32)[0:1]
        part = rows_ref[j, 0:rows, :].astype(jnp.float32)
        normed[:, j * local : (j + 1) * local] = (part * scale * gain).astype(jnp.bfloat16)
    for n in range(given - 1):
        last = given if n == given - 2 else n + 1
        both = lax.dot_general(
            normed[...],
            jnp.concatenate([ref[...] for ref in (*gates[n:last], *ups[n:last])], axis=0),
            (((1,), (1,)), ((), ())),
            preferred_element_type=jnp.float32,
        )
        gate, up = both[:, :units], both[:, units:]
        hidden = (gate / (1.0 + jnp.exp(-gate)) * up).astype(jnp.bfloat16)
        for p in range(out_ref.shape[0]):
            out_ref[p, :, n * units : (n + 1) * units] = hidden


def down_kernel(idx_ref, hidden_ref, *refs, pieces):
    weights = refs[:pieces]
    outs = refs[pieces : 2 * pieces]
    ordered = refs[2 * pieces]
    units = hidden_ref.shape[2] // pieces
    for p in range(hidden_ref.shape[0]):
        for n in range(pieces):
            at = pl.multiple_of(idx_ref[p * pieces + n] * units, units)
            part = hidden_ref[p, :, n * units : (n + 1) * units]
            if n == pieces - 1:
                other = hidden_ref[p ^ 2, :, n * units : (n + 1) * units]
                lane = lax.broadcasted_iota(jnp.int32, part.shape, 1)
                part = jnp.where(
                    lane < units // 2, part.astype(jnp.float32), other.astype(jnp.float32)
                ).astype(jnp.bfloat16)
            ordered[:, pl.ds(at, units)] = part
    for n in range(pieces):
        outs[n][...] = jnp.dot(
            ordered[...], weights[n][...], preferred_element_type=jnp.float32
        ).astype(jnp.bfloat16)


def gather_kernel(q_ref, *refs):
    out_ref = refs[-1]
    for i, ref in enumerate(refs[:-1]):
        out_ref[q_ref[i]] = ref[...]


def in_hbm(value):
    return pltpu.with_memory_space_constraint(value, pltpu.HBM)


def in_vmem(value):
    return pltpu.with_memory_space_constraint(value, pltpu.VMEM)


def body(tokens, norm_gain, expert_ids, combine_weight, w_gate, w_up, w_down, out_gain):
    tok_rows, local = tokens.shape
    n_split = lax.axis_size("ep")
    n_route = lax.axis_size("tp")
    width = local * n_split
    experts = w_gate.shape[0] * n_route
    capacity = 2 * expert_ids.shape[1] * tok_rows // experts
    slots = experts * capacity
    rows = n_route * capacity // CLASSES
    units = w_gate.shape[1]
    hidden_all = units * n_split
    w_gate, w_up, w_down = w_gate[0], w_up[0], w_down[0]
    vmem = pl.BlockSpec(memory_space=pltpu.VMEM)
    ids = expert_ids.T

    smem = pl.BlockSpec(memory_space=pltpu.SMEM)
    core = lax.axis_index("tp") % 2
    me = lax.axis_index("ep")
    place = jnp.where(core == 0, me, turn(me, 1))
    mine = klass(place)
    class_of = jnp.asarray(
        [[klass(turn(i, k)) for i in range(n_split)] for k in range(2)], jnp.int32
    )
    class_of = lax.dynamic_index_in_dim(class_of, core, 0, keepdims=False)
    buffer = pl.pallas_call(
        functools.partial(dispatch_kernel, experts=experts, capacity=capacity),
        out_shape=jax.ShapeDtypeStruct((slots, local), jnp.bfloat16),
        in_specs=[vmem, vmem],
        out_specs=vmem,
        scratch_shapes=[pltpu.VMEM((slots, tok_rows), jnp.bfloat16)],
        compiler_params=pltpu.CompilerParams(vmem_limit_bytes=GRANT),
        name="dispatch",
    )(in_hbm(ids), in_hbm(tokens))
    arrived = lax.all_to_all(
        buffer.reshape(experts, capacity, local),
        "tp",
        split_axis=0,
        concat_axis=0,
        tiled=True,
    )

    steps = ((0, 1), (0, -1))
    last_steps = ((0, 1), (0, -1), (1, 0))
    gates = spread_weights(w_gate, steps)
    ups = spread_weights(w_up, steps)
    downs = [w_down, *(shifted(w_down, *s) for s in last_steps)]
    given, pieces = len(gates), len(downs)

    picks, weights = pl.pallas_call(
        functools.partial(prepare_kernel, experts=experts, capacity=capacity),
        out_shape=[
            pltpu.VMEM((expert_ids.shape[1], tok_rows, slots), jnp.bfloat16),
            pltpu.VMEM((expert_ids.shape[1], tok_rows, 128), jnp.float32),
        ],
        in_specs=[vmem, vmem],
        out_specs=[vmem, vmem],
        compiler_params=pltpu.CompilerParams(vmem_limit_bytes=GRANT),
        name="prepare",
    )(ids, combine_weight.T)
    operand = pl.pallas_call(
        spread_kernel,
        out_shape=jax.ShapeDtypeStruct((n_split, rows + EXTRA, local), jnp.bfloat16),
        in_specs=[smem, vmem, vmem],
        out_specs=vmem,
        compiler_params=pltpu.CompilerParams(vmem_limit_bytes=GRANT),
        name="spread",
    )(class_of, in_vmem(arrived.reshape(CLASSES, rows, local)), norm_gain[None, :])
    gathered = lax.all_to_all(operand, "ep", split_axis=0, concat_axis=0, tiled=True)

    hidden = pl.pallas_call(
        functools.partial(up_kernel, given=given, width=width),
        out_shape=pltpu.HBM((SIDE, rows, pieces * units), jnp.bfloat16),
        in_specs=[vmem] * (1 + 2 * given),
        out_specs=vmem,
        scratch_shapes=[pltpu.VMEM((rows, width), jnp.bfloat16)],
        compiler_params=pltpu.CompilerParams(vmem_limit_bytes=GRANT),
        name="gate_up",
    )(in_vmem(gathered), *(in_vmem(w) for w in (*gates, *ups)))

    groups = [
        [
            [turn(v, k) for v in range(n_split) if klass(v) == q]
            for q in range(CLASSES)
        ]
        for k in range(2)
    ]
    shared = lax.all_to_all(
        hidden,
        ("ep", "tp"),
        split_axis=0,
        concat_axis=0,
        tiled=True,
        axis_index_groups=[
            [i * n_route + t for i in group]
            for t in range(n_route)
            for group in groups[t % 2]
        ],
    )
    table = jnp.asarray(
        [
            [
                [
                    turn(v, k)
                    for i in group
                    for v in (
                        turn(i, k),
                        *(moved(turn(i, k), -dy, -dx) for dy, dx in steps),
                        moved(turn(i, k), 1, 0),
                    )
                ]
                for group in groups[k]
            ]
            for k in range(2)
        ],
        jnp.int32,
    ).reshape(2 * CLASSES, SIDE * pieces)
    order = lax.dynamic_index_in_dim(table, core * CLASSES + mine, 0, keepdims=False)

    outs = pl.pallas_call(
        functools.partial(down_kernel, pieces=pieces),
        out_shape=[pltpu.VMEM((rows, local), jnp.bfloat16)] * pieces,
        in_specs=[smem] + [vmem] * (1 + pieces),
        out_specs=[vmem] * pieces,
        scratch_shapes=[pltpu.VMEM((rows, hidden_all), jnp.bfloat16)],
        compiler_params=pltpu.CompilerParams(vmem_limit_bytes=GRANT),
        name="down",
    )(order, in_vmem(shared), *(in_vmem(w) for w in downs))

    pieces_back = [
        outs[0],
        *(shifted(out, -dy, -dx) for out, (dy, dx) in zip(outs[1:], last_steps)),
    ]
    places = jnp.asarray([0, *(dx + 2 * dy for dy, dx in last_steps)], jnp.int32)
    places = (mine + places) % CLASSES
    returned = pl.pallas_call(
        gather_kernel,
        out_shape=pltpu.VMEM((CLASSES, rows, local), jnp.bfloat16),
        in_specs=[smem] + [vmem] * pieces,
        out_specs=vmem,
        compiler_params=pltpu.CompilerParams(vmem_limit_bytes=GRANT),
        name="gather",
    )(places, *(in_vmem(piece) for piece in pieces_back))

    answers = lax.all_to_all(
        returned.reshape(n_route, capacity, local),
        "tp",
        split_axis=0,
        concat_axis=0,
        tiled=True,
    )
    moe, squares = pl.pallas_call(
        combine_kernel,
        out_shape=[
            pltpu.VMEM((tok_rows, local), jnp.float32),
            pltpu.VMEM((n_split, 1, tok_rows), jnp.float32),
        ],
        in_specs=[vmem] * 3,
        out_specs=[vmem] * 2,
        compiler_params=pltpu.CompilerParams(vmem_limit_bytes=GRANT),
        name="combine",
    )(in_vmem(picks), in_vmem(weights), in_vmem(answers.reshape(slots, local)))
    squares = lax.all_to_all(squares, "ep", split_axis=0, concat_axis=0, tiled=True)
    total = jnp.sum(squares, axis=(0, 1))
    mixed = (
        moe
        * lax.rsqrt(total / width + epsilon)[:, None]
        * out_gain.astype(jnp.float32)[None, :]
    )
    return mixed.astype(jnp.bfloat16)


def solution(mesh):
    return jax.shard_map(
        body,
        mesh=mesh,
        in_specs=(
            P("tp", "ep"),
            P("ep"),
            P("tp", None),
            P("tp", None),
            P("tp", "ep", None),
            P("tp", "ep", None),
            P("tp", None, "ep"),
            P("ep"),
        ),
        out_specs=P("tp", "ep"),
        check_vma=False,
    )
```

```python
import functools

import jax
import jax.numpy as jnp
from jax import lax
from jax.experimental import pallas as pl
from jax.experimental.pallas import tpu as pltpu
from jax.sharding import PartitionSpec as P


SIDE = 4
CLASSES = 4
EXTRA = 16
epsilon = 1e-06


GRANT = 24 * 1024 * 1024


def turn(i, core):
    return i if core == 0 else i % SIDE * SIDE + i // SIDE


def klass(i):
    return (i % SIDE + 2 * (i // SIDE)) % CLASSES


def moved(i, dy, dx):
    return (i // SIDE + dy) % SIDE * SIDE + (i % SIDE + dx) % SIDE


def shifted(value, dy, dx):
    n_route = lax.axis_size("tp")
    pairs = []
    for i in range(SIDE * SIDE):
        for t in range(n_route):
            to = turn(moved(turn(i, t % 2), dy, dx), t % 2)
            pairs.append((i * n_route + t, to * n_route + t))
    return lax.ppermute(value, ("ep", "tp"), pairs)


def spread_weights(weight, steps):
    half = weight.shape[0] // 2
    return [
        weight,
        *(shifted(weight, *s) for s in steps),
        shifted(weight[:half], -1, 0),
        shifted(weight[half:], 1, 0),
    ]


def slots_of(ids, experts):
    tokens = ids.shape[1]
    expert = lax.broadcasted_iota(jnp.int32, (experts, tokens), 0)
    first, second = ids[0:1] == expert, ids[1:2] == expert
    named = jnp.logical_or(first, second)
    before = lax.broadcasted_iota(jnp.int32, (tokens, tokens), 0) < lax.broadcasted_iota(
        jnp.int32, (tokens, tokens), 1
    )
    rank = jnp.dot(
        named.astype(jnp.float32).astype(jnp.bfloat16),
        before.astype(jnp.float32).astype(jnp.bfloat16),
        preferred_element_type=jnp.float32,
    )
    return first, second, jnp.where(named, rank, -1.0)


def dispatch_kernel(ids_ref, x_ref, out_ref, pick_ref, *, experts, capacity):
    tokens = x_ref.shape[0]
    _, _, slot = slots_of(ids_ref[...], experts)
    place = lax.broadcasted_iota(jnp.int32, (capacity, tokens), 0).astype(jnp.float32)
    for e in range(experts):
        pick = (slot[e : e + 1] == place).astype(jnp.float32).astype(jnp.bfloat16)
        pick_ref[e * capacity : (e + 1) * capacity] = pick
    out_ref[...] = jnp.dot(
        pick_ref[...], x_ref[...], preferred_element_type=jnp.float32
    ).astype(jnp.bfloat16)


def prepare_kernel(ids_ref, w_ref, pick_ref, out_ref, *, experts, capacity):
    first, second, slot = slots_of(ids_ref[...], experts)
    tall = out_ref.shape[1:][::-1]
    base = lax.broadcasted_iota(jnp.int32, slot.shape, 0).astype(jnp.float32) * capacity
    place = lax.broadcasted_iota(jnp.int32, pick_ref.shape[1:], 1).astype(jnp.float32)
    for k, mine in enumerate((first, second)):
        target = jnp.sum(jnp.where(mine, base + slot, 0.0), axis=0, keepdims=True)
        target = jnp.broadcast_to(target, tall).T[:, 0:1]
        pick_ref[k] = (place == target).astype(jnp.float32).astype(jnp.bfloat16)
    for k in range(w_ref.shape[0]):
        out_ref[k] = jnp.broadcast_to(w_ref[k : k + 1], tall).T


def combine_kernel(pick_ref, w_ref, back_ref, moe_ref, sq_ref):
    routes, tokens, slots = pick_ref.shape
    picked = jnp.dot(
        pick_ref[...].reshape(routes * tokens, slots),
        back_ref[...],
        preferred_element_type=jnp.float32,
    )
    moe = None
    for k in range(routes):
        term = picked[k * tokens : (k + 1) * tokens] * w_ref[k][:, 0:1]
        moe = term if moe is None else moe + term
    moe_ref[...] = moe
    squares = jnp.sum(moe * moe, axis=1, keepdims=True)
    squares = jnp.broadcast_to(squares, (tokens, 128)).T
    for i in range(sq_ref.shape[0]):
        sq_ref[i] = squares[0:1]


def spread_kernel(q_ref, rows_ref, gain_ref, out_ref):
    rows = rows_ref.shape[1]
    gain = jnp.broadcast_to(gain_ref[...].astype(jnp.float32), (EXTRA, rows_ref.shape[2]))
    gain = gain.astype(jnp.bfloat16)
    for i in range(out_ref.shape[0]):
        out_ref[i, 0:rows, :] = rows_ref[q_ref[i]]
        out_ref[i, rows : rows + EXTRA, :] = gain


def up_kernel(*refs, given, width):
    rows_ref = refs[0]
    gates, ups = refs[1 : 1 + given], refs[1 + given : 1 + 2 * given]
    out_ref, normed = refs[1 + 2 * given :]
    sources, _, local = rows_ref.shape
    units = gates[0].shape[0]
    rows = normed.shape[0]
    squares = jnp.zeros((rows, local), jnp.float32)
    for j in range(sources):
        part = rows_ref[j, 0:rows, :].astype(jnp.float32)
        squares = squares + part * part
    scale = lax.rsqrt(jnp.sum(squares, axis=1, keepdims=True) / width + epsilon)
    for j in range(sources):
        gain = rows_ref[j, rows : rows + EXTRA, :].astype(jnp.float32)[0:1]
        part = rows_ref[j, 0:rows, :].astype(jnp.float32)
        normed[:, j * local : (j + 1) * local] = (part * scale * gain).astype(jnp.bfloat16)
    for n in range(given - 1):
        last = given if n == given - 2 else n + 1
        both = lax.dot_general(
            normed[...],
            jnp.concatenate([ref[...] for ref in (*gates[n:last], *ups[n:last])], axis=0),
            (((1,), (1,)), ((), ())),
            preferred_element_type=jnp.float32,
        )
        gate, up = both[:, :units], both[:, units:]
        hidden = (gate / (1.0 + jnp.exp(-gate)) * up).astype(jnp.bfloat16)
        for p in range(out_ref.shape[0]):
            out_ref[p, :, n * units : (n + 1) * units] = hidden


def down_kernel(idx_ref, hidden_ref, *refs, pieces):
    weights = refs[: pieces - 1]
    outs = refs[pieces - 1 : 2 * pieces - 2]
    ordered = refs[2 * pieces - 2]
    units = hidden_ref.shape[2] // pieces
    for p in range(hidden_ref.shape[0]):
        for n in range(pieces):
            at = pl.multiple_of(idx_ref[p * pieces + n] * units, units)
            part = hidden_ref[p, :, n * units : (n + 1) * units]
            if n == pieces - 1:
                other = hidden_ref[p ^ 2, :, n * units : (n + 1) * units]
                lane = lax.broadcasted_iota(jnp.int32, part.shape, 1)
                part = jnp.where(
                    lane < units // 2, part.astype(jnp.float32), other.astype(jnp.float32)
                ).astype(jnp.bfloat16)
            ordered[:, pl.ds(at, units)] = part
    for n in range(pieces - 1):
        outs[n][...] = jnp.dot(
            ordered[...], weights[n][...], preferred_element_type=jnp.float32
        ).astype(jnp.bfloat16)


def own_kernel(ordered_ref, weight_ref, out_ref):
    out_ref[...] = jnp.dot(
        ordered_ref[...], weight_ref[...], preferred_element_type=jnp.float32
    ).astype(jnp.bfloat16)


def gather_kernel(q_ref, *refs):
    out_ref = refs[-1]
    for i, ref in enumerate(refs[:-1]):
        out_ref[q_ref[i]] = ref[...]


def in_hbm(value):
    return pltpu.with_memory_space_constraint(value, pltpu.HBM)


def in_vmem(value):
    return pltpu.with_memory_space_constraint(value, pltpu.VMEM)


def body(tokens, norm_gain, expert_ids, combine_weight, w_gate, w_up, w_down, out_gain):
    tok_rows, local = tokens.shape
    n_split = lax.axis_size("ep")
    n_route = lax.axis_size("tp")
    width = local * n_split
    experts = w_gate.shape[0] * n_route
    capacity = 2 * expert_ids.shape[1] * tok_rows // experts
    slots = experts * capacity
    rows = n_route * capacity // CLASSES
    units = w_gate.shape[1]
    hidden_all = units * n_split
    w_gate, w_up, w_down = w_gate[0], w_up[0], w_down[0]
    vmem = pl.BlockSpec(memory_space=pltpu.VMEM)
    ids = expert_ids.T

    smem = pl.BlockSpec(memory_space=pltpu.SMEM)
    core = lax.axis_index("tp") % 2
    me = lax.axis_index("ep")
    place = jnp.where(core == 0, me, turn(me, 1))
    mine = klass(place)
    class_of = jnp.asarray(
        [[klass(turn(i, k)) for i in range(n_split)] for k in range(2)], jnp.int32
    )
    class_of = lax.dynamic_index_in_dim(class_of, core, 0, keepdims=False)
    buffer = pl.pallas_call(
        functools.partial(dispatch_kernel, experts=experts, capacity=capacity),
        out_shape=jax.ShapeDtypeStruct((slots, local), jnp.bfloat16),
        in_specs=[vmem, vmem],
        out_specs=vmem,
        scratch_shapes=[pltpu.VMEM((slots, tok_rows), jnp.bfloat16)],
        compiler_params=pltpu.CompilerParams(vmem_limit_bytes=GRANT),
        name="dispatch",
    )(in_hbm(ids), in_hbm(tokens))
    arrived = lax.all_to_all(
        buffer.reshape(experts, capacity, local),
        "tp",
        split_axis=0,
        concat_axis=0,
        tiled=True,
    )

    steps = ((0, 1), (0, -1))
    last_steps = ((0, 1), (0, -1), (1, 0))
    gates = spread_weights(w_gate, steps)
    ups = spread_weights(w_up, steps)
    downs = [w_down, *(shifted(w_down, *s) for s in last_steps)]
    given, pieces = len(gates), len(downs)

    picks, weights = pl.pallas_call(
        functools.partial(prepare_kernel, experts=experts, capacity=capacity),
        out_shape=[
            pltpu.VMEM((expert_ids.shape[1], tok_rows, slots), jnp.bfloat16),
            pltpu.VMEM((expert_ids.shape[1], tok_rows, 128), jnp.float32),
        ],
        in_specs=[vmem, vmem],
        out_specs=[vmem, vmem],
        compiler_params=pltpu.CompilerParams(vmem_limit_bytes=GRANT),
        name="prepare",
    )(ids, combine_weight.T)
    operand = pl.pallas_call(
        spread_kernel,
        out_shape=jax.ShapeDtypeStruct((n_split, rows + EXTRA, local), jnp.bfloat16),
        in_specs=[smem, vmem, vmem],
        out_specs=vmem,
        compiler_params=pltpu.CompilerParams(vmem_limit_bytes=GRANT),
        name="spread",
    )(class_of, in_vmem(arrived.reshape(CLASSES, rows, local)), norm_gain[None, :])
    gathered = lax.all_to_all(operand, "ep", split_axis=0, concat_axis=0, tiled=True)

    hidden = pl.pallas_call(
        functools.partial(up_kernel, given=given, width=width),
        out_shape=pltpu.HBM((SIDE, rows, pieces * units), jnp.bfloat16),
        in_specs=[vmem] * (1 + 2 * given),
        out_specs=vmem,
        scratch_shapes=[pltpu.VMEM((rows, width), jnp.bfloat16)],
        compiler_params=pltpu.CompilerParams(vmem_limit_bytes=GRANT),
        name="gate_up",
    )(in_vmem(gathered), *(in_vmem(w) for w in (*gates, *ups)))

    groups = [
        [
            [turn(v, k) for v in range(n_split) if klass(v) == q]
            for q in range(CLASSES)
        ]
        for k in range(2)
    ]
    shared = lax.all_to_all(
        hidden,
        ("ep", "tp"),
        split_axis=0,
        concat_axis=0,
        tiled=True,
        axis_index_groups=[
            [i * n_route + t for i in group]
            for t in range(n_route)
            for group in groups[t % 2]
        ],
    )
    table = jnp.asarray(
        [
            [
                [
                    turn(v, k)
                    for i in group
                    for v in (
                        turn(i, k),
                        *(moved(turn(i, k), -dy, -dx) for dy, dx in steps),
                        moved(turn(i, k), 1, 0),
                    )
                ]
                for group in groups[k]
            ]
            for k in range(2)
        ],
        jnp.int32,
    ).reshape(2 * CLASSES, SIDE * pieces)
    order = lax.dynamic_index_in_dim(table, core * CLASSES + mine, 0, keepdims=False)

    *outs, ordered = pl.pallas_call(
        functools.partial(down_kernel, pieces=pieces),
        out_shape=[
            *[pltpu.VMEM((rows, local), jnp.bfloat16)] * (pieces - 1),
            pltpu.VMEM((rows, hidden_all), jnp.bfloat16),
        ],
        in_specs=[smem] + [vmem] * pieces,
        out_specs=[vmem] * pieces,
        compiler_params=pltpu.CompilerParams(vmem_limit_bytes=GRANT),
        name="down",
    )(order, in_vmem(shared), *(in_vmem(w) for w in downs[1:]))
    backs = [shifted(out, -dy, -dx) for out, (dy, dx) in zip(outs, last_steps)]
    own = pl.pallas_call(
        own_kernel,
        out_shape=pltpu.VMEM((rows, local), jnp.bfloat16),
        in_specs=[vmem] * 2,
        out_specs=vmem,
        compiler_params=pltpu.CompilerParams(vmem_limit_bytes=GRANT),
        name="own",
    )(in_vmem(ordered), in_vmem(downs[0]))
    pieces_back = [own, *backs]
    places = jnp.asarray([0, *(dx + 2 * dy for dy, dx in last_steps)], jnp.int32)
    places = (mine + places) % CLASSES
    returned = pl.pallas_call(
        gather_kernel,
        out_shape=pltpu.VMEM((CLASSES, rows, local), jnp.bfloat16),
        in_specs=[smem] + [vmem] * pieces,
        out_specs=vmem,
        compiler_params=pltpu.CompilerParams(vmem_limit_bytes=GRANT),
        name="gather",
    )(places, *(in_vmem(piece) for piece in pieces_back))

    answers = lax.all_to_all(
        returned.reshape(n_route, capacity, local),
        "tp",
        split_axis=0,
        concat_axis=0,
        tiled=True,
    )
    moe, squares = pl.pallas_call(
        combine_kernel,
        out_shape=[
            pltpu.VMEM((tok_rows, local), jnp.float32),
            pltpu.VMEM((n_split, 1, tok_rows), jnp.float32),
        ],
        in_specs=[vmem] * 3,
        out_specs=[vmem] * 2,
        compiler_params=pltpu.CompilerParams(vmem_limit_bytes=GRANT),
        name="combine",
    )(in_vmem(picks), in_vmem(weights), in_vmem(answers.reshape(slots, local)))
    squares = lax.all_to_all(squares, "ep", split_axis=0, concat_axis=0, tiled=True)
    total = jnp.sum(squares, axis=(0, 1))
    mixed = (
        moe
        * lax.rsqrt(total / width + epsilon)[:, None]
        * out_gain.astype(jnp.float32)[None, :]
    )
    return mixed.astype(jnp.bfloat16)


def solution(mesh):
    return jax.shard_map(
        body,
        mesh=mesh,
        in_specs=(
            P("tp", "ep"),
            P("ep"),
            P("tp", None),
            P("tp", None),
            P("tp", "ep", None),
            P("tp", "ep", None),
            P("tp", None, "ep"),
            P("ep"),
        ),
        out_specs=P("tp", "ep"),
        check_vma=False,
    )
```
